32 devices in a mesh: sp: 8 (over z, x), tp: 4 (over y, core).
Axes of the slice: x: 2, y: 2, z: 4, core: 2. Of those that a mesh axis runs over, the one named last changes fastest.
Arguments:
- resid: bfloat16 [4096, 2048], P(('sp', 'tp')), may hold values from -6 to 6
- pool_in: bfloat16 [4096, 1024], P('sp', 'tp'), may hold values from -8 to 8
- doc_ids: int32 [4096], P('sp'), may hold values from 0 to 3, never falling along the last dimension, each value on 1 to 1536 neighbouring positions
- w_group: bfloat16 [8, 128, 128], replicated, may hold values from -0.5 to 0.5
- pool_scale: bfloat16 [1024], replicated, may hold values from 0.099609375 to 1.8984375
- w_branch: bfloat16 [1024, 2048], P('tp'), may hold values from -0.1875 to 0.1875
- norm_gain: bfloat16 [2048], replicated, may hold values from 0.099609375 to 1.8984375
- route_ids: int32 [4096, 4], P(('sp', 'tp')), may hold values from 0 to 31, all different within a row; in each aligned block of 128 rows (0 to 127, 128 to 255, ...) at most 32 rows name the same one
- route_wts: float32 [4096, 4], P(('sp', 'tp')), may hold values from 0.2 to 1
- w_exp_gate: bfloat16 [32, 2048, 512], P(('sp', 'tp')), may hold values from -0.125 to 0.125
- w_exp_up: bfloat16 [32, 2048, 512], P(('sp', 'tp')), may hold values from -0.125 to 0.125
- w_exp_down: bfloat16 [32, 512, 2048], P(('sp', 'tp')), may hold values from -0.25 to 0.25
- w_sh_gate: bfloat16 [2048, 512], replicated, may hold values from -0.125 to 0.125
- w_sh_up: bfloat16 [2048, 512], replicated, may hold values from -0.125 to 0.125
- w_sh_down: bfloat16 [512, 2048], replicated, may hold values from -0.25 to 0.25
- final_gain: bfloat16 [2048], replicated, may hold values from 0.099609375 to 1.8984375
Outputs:
- final: bfloat16 [4096, 2048], P(('sp', 'tp'))
The draws below stay inside these ranges and needn't reach their ends.
Inputs may be any that keep to these rules, and one draw needn't show every extreme that they name: `doc_ids`: never falls along the positions. `route_ids`: each row names 4 different experts; among the rows of one device (aligned blocks of 128 rows) no expert is named by more than 32 rows, a bound that some block reaches.
All inputs are finite; a program needn't handle non-finite values.
Results may differ from the reference program's by a relative error of at most 0.0062.
Values may be sent and summed in bfloat16 or wider, within the bound.
A program may use at most 128 MiB of HBM per device.

```python
import math
import jax
import jax.numpy as jnp
import numpy as np
from jax import lax

D = 2048
GROUP_CH = 128
GROUPS = 8
FF = 512
TOPK = 4
ROWS = 128
P_SIZE = 1024
EXPERTS = 32
TOK_DEV = 512
TOKENS = 4096
CAP = 32
N_SP = 8
DEVICES = 32


def draw_pool_in(key, part):
    offset_key = jax.random.fold_in(key, 11)
    noise_key = jax.random.fold_in(key, 12)
    block_count = TOKENS // 64
    offsets = jnp.clip(jax.random.normal(offset_key, (block_count, P_SIZE), jnp.float32) * 1.5, -4.0, 4.0)
    cell_noise = jnp.clip(jax.random.normal(noise_key, (TOKENS, P_SIZE), jnp.float32), -4.0, 4.0)
    return (jnp.repeat(offsets, 64, axis=0) + cell_noise).astype(jnp.bfloat16)


def block_scale(rng, dims, pieces, least, largest):
    loudness = 1.0
    for axis_at, shards_of in pieces:
        steps = jax.random.uniform(jax.random.fold_in(jax.random.fold_in(rng, 6), axis_at), (shards_of,), jnp.float32, least / len(pieces), largest / len(pieces))
        loudness = loudness * jnp.repeat(jnp.exp(steps), dims[axis_at] // shards_of).reshape((-1,) + (1,) * (len(dims) - 1 - axis_at))
    return loudness


def profile(count, total, bound, skew):
    portions = [(1 << 20) // math.isqrt(standing ** skew) + 1 for standing in range(2, count + 1)]
    rest, given = total - bound - (count - 1), [1] * (count - 1)
    while rest > 0:
        free = [i for i in range(count - 1) if given[i] < bound]
        mass, budget = sum([portions[i] for i in free]), rest
        for i in free:
            more = min(bound - given[i], max(1, budget * portions[i] // mass), rest)
            given[i] = given[i] + more
            rest = rest - more
    return np.array([bound] + given)


def uneven_parts(stream_key, amount, total, reach, lean):
    if amount == 2:
        one = jax.random.randint(stream_key, (), max(1, total - reach), min(reach, total - 1) + 1)
        return jnp.stack([one, total - one])
    sizes = jnp.asarray(profile(amount, total, reach, lean), jnp.int32)
    pairs = (amount - 1) // 2
    donor, receiver = sizes[1:1 + 2 * pairs:2], sizes[2:2 + 2 * pairs:2]
    slack = jnp.minimum(donor - 1, reach - receiver)
    passed = jax.random.randint(jax.random.fold_in(stream_key, 1), (pairs,), 0, 1 << 20) % (slack + 1)
    sizes = sizes.at[1:1 + 2 * pairs:2].set(donor - passed).at[2:2 + 2 * pairs:2].set(receiver + passed)
    return sizes[jax.random.permutation(jax.random.fold_in(stream_key, 2), amount)]


def assign_block(key, own, number, rows, number_of, top, reach, slope):
    sequence = jax.random.permutation(key, number_of)
    packed, common = portions_of(number_of, rows * top, reach, slope, True), portions_of(number_of, rows * top, reach, slope, False)
    places = jnp.arange(number_of)

    def named(sizes, offset_by):
        used = int((sizes > 0).sum())
        fixed = max(1, used // 4)
        passed = fixed + (places - fixed + offset_by * (used - fixed)) % max(1, number_of - fixed)
        return jnp.zeros((number_of,), jnp.int32).at[sequence[jnp.where(places < fixed, places, passed)]].set(jnp.asarray(sizes, jnp.int32))

    sizes = jnp.where(number % 4 == 0, named(packed, number // 4), named(common, number - number // 4 - 1))
    mixed = jax.random.permutation(jax.random.fold_in(own, 3), number_of)
    source_of, taker = mixed[0:number_of // 2 * 2:2], mixed[1:number_of // 2 * 2:2]
    slack = jnp.minimum(sizes[source_of] - 1, reach - sizes[taker]) // 2
    slack = jnp.where((source_of == sequence[0]) | (taker == sequence[0]) | (sizes[taker] == 0), 0, jnp.maximum(slack, 0))
    passed = jax.random.randint(jax.random.fold_in(own, 4), (number_of // 2,), 0, 1 << 20) % (slack + 1)
    sizes = sizes.at[source_of].add(-passed).at[taker].add(passed)
    labels = jnp.searchsorted(jnp.cumsum(sizes), jnp.arange(rows * top), side="right").astype(jnp.int32)
    grid = labels.reshape(top, rows).T
    grid = grid[jax.random.permutation(jax.random.fold_in(own, 1), rows)]
    offset_by = jax.random.randint(jax.random.fold_in(own, 2), (rows, 1), 0, top)
    return jnp.take_along_axis(grid, (jnp.arange(top)[None, :] + offset_by) % top, axis=1)


def portions_of(amount, total, limit, lean, full):
    portions = [(1 << 20) // math.isqrt(standing ** lean) + 1 for standing in range(1, amount + 1)]
    largest = limit if full else min(limit, max(-(-total // amount), total * portions[0] // sum(portions)))
    least = 1 if total - largest >= amount - 1 else 0
    holding, spare = [largest] + [least] * (amount - 1), total - largest - least * (amount - 1)
    while spare > 0:
        free = [i for i in range(1, amount) if holding[i] < largest] or [i for i in range(1, amount) if holding[i] < limit]
        mass, left = sum([portions[i] for i in free]), spare
        for i in free:
            extra = min(limit - holding[i], max(1, left * portions[i] // mass), spare)
            holding[i] = holding[i] + extra
            spare = spare - extra
    return np.array(holding)


def noise(rng, extent, width, bound, shards=(), kind=jnp.bfloat16):
    result = width * jax.random.normal(rng, extent, jnp.float32)
    if shards:
        result = result * block_scale(rng, extent, shards, -0.22, 0.18)
    return jnp.clip(result, -bound, bound).astype(kind)


def setup_inputs(seed: int = 0) -> dict:
    arg_keys = jax.random.split(jax.random.key(seed), 17)
    resid = noise(arg_keys[0], (TOKENS, D), 1.0, 6.0, ((0, 32),))
    pool_in = draw_pool_in(jax.random.fold_in(arg_keys[16], 71), 0)
    doc_ids = jnp.searchsorted(jnp.cumsum(uneven_parts(arg_keys[2], N_SP // 2, TOKENS, 3 * TOK_DEV, 1)), jnp.arange(TOKENS), side="right").astype(jnp.int32)
    w_group = noise(arg_keys[3], (GROUPS, GROUP_CH, GROUP_CH), GROUP_CH ** -0.5, 0.5)
    pool_scale = jnp.clip(1.0 + 0.18 * jax.random.normal(arg_keys[4], (P_SIZE,), jnp.float32), 0.099609375, 1.8984375).astype(jnp.bfloat16)
    w_branch = noise(arg_keys[5], (P_SIZE, D), P_SIZE ** -0.5, 0.1875, ((0, 4),))
    norm_gain = jnp.clip(1.0 + 0.18 * jax.random.normal(arg_keys[6], (D,), jnp.float32), 0.099609375, 1.8984375).astype(jnp.bfloat16)
    route_ids_keys = jax.random.split(jax.random.fold_in(arg_keys[7], 1), TOKENS // ROWS)
    route_ids_turns = jax.random.permutation(jax.random.fold_in(arg_keys[7], 3), TOKENS // ROWS)
    route_ids = jax.vmap(lambda own, number: assign_block(jax.random.fold_in(arg_keys[7], 2), own, number, ROWS, EXPERTS, TOPK, CAP, 2))(route_ids_keys, route_ids_turns).reshape((TOKENS, TOPK))
    route_wts = jnp.clip(0.2 + 0.8 * jax.random.uniform(arg_keys[8], (TOKENS, TOPK), jnp.float32) ** block_scale(arg_keys[8], (TOKENS, TOPK), ((0, 32),), -0.2, 0.2), 0.2, 1.0)
    w_exp_gate = noise(arg_keys[9], (EXPERTS, D, FF), D ** -0.5, 0.125, ((0, 32),))
    w_exp_up = noise(arg_keys[10], (EXPERTS, D, FF), D ** -0.5, 0.125, ((0, 32),))
    w_exp_down = noise(arg_keys[11], (EXPERTS, FF, D), FF ** -0.5, 0.25, ((0, 32),))
    w_sh_gate = noise(arg_keys[12], (D, FF), D ** -0.5, 0.125)
    w_sh_up = noise(arg_keys[13], (D, FF), D ** -0.5, 0.125)
    w_sh_down = noise(arg_keys[14], (FF, D), FF ** -0.5, 0.25)
    final_gain = jnp.clip(1.0 + 0.18 * jax.random.normal(arg_keys[15], (D,), jnp.float32), 0.099609375, 1.8984375).astype(jnp.bfloat16)
    return {"resid": resid, "pool_in": pool_in, "doc_ids": doc_ids, "w_group": w_group, "pool_scale": pool_scale, "w_branch": w_branch, "norm_gain": norm_gain, "route_ids": route_ids, "route_wts": route_wts, "w_exp_gate": w_exp_gate, "w_exp_up": w_exp_up, "w_exp_down": w_exp_down, "w_sh_gate": w_sh_gate, "w_sh_up": w_sh_up, "w_sh_down": w_sh_down, "final_gain": final_gain}


pool_windows = (2, 4, 8, 16, 16, 32, 64, 128)
alpha_mix = 8.0 ** 0.25
norm_eps = 1e-05

def layer_norm(values, scales):
    center = values - lax.optimization_barrier(jnp.mean(values, axis=-1, keepdims=True))
    spread = lax.optimization_barrier(jnp.mean(center * center, axis=-1, keepdims=True))
    return center * lax.rsqrt(spread + norm_eps) * scales.astype(jnp.float32)

def channel_windows(channel_count, group_width):
    groups = jnp.arange(channel_count, dtype=jnp.int32) // group_width
    window_table = jnp.asarray(pool_windows, dtype=jnp.int32)
    matches = groups[:, None] == jnp.arange(len(pool_windows), dtype=jnp.int32)[None, :]
    return lax.optimization_barrier(jnp.sum(jnp.where(matches, window_table[None, :], 0), axis=1)).astype(jnp.float32)

def swiglu_hidden(token_rows, gate_weight, up_weight):
    gate_vals = jnp.dot(token_rows, gate_weight, preferred_element_type=jnp.float32)
    up_vals = jnp.dot(token_rows, up_weight, preferred_element_type=jnp.float32)
    return (jax.nn.silu(gate_vals) * up_vals).astype(jnp.bfloat16)

def reference(resid, pool_in, doc_ids, w_group, pool_scale, w_branch, norm_gain, route_ids, route_wts, w_exp_gate, w_exp_up, w_exp_down, w_sh_gate, w_sh_up, w_sh_down, final_gain):
    values = pool_in.astype(jnp.float32)
    positions = jnp.arange(TOKENS, dtype=jnp.int32)
    change = jnp.concatenate([jnp.ones((1,), bool), doc_ids[1:] != doc_ids[:-1]])
    doc_start = lax.cummax(jnp.where(change, positions, 0), axis=0)
    since_start = (positions - doc_start).astype(jnp.float32)[:, None]
    cumulative = jnp.concatenate([jnp.zeros((1, P_SIZE), jnp.float32), jnp.cumsum(values, axis=0)], axis=0)
    current = cumulative[1:]
    running = current - cumulative[doc_start]
    doc_mean = running / (since_start + 1.0)
    widths = channel_windows(P_SIZE, GROUP_CH)[None, :]
    recent = running
    for window in sorted(set(pool_windows)):
        lagged = jnp.concatenate([jnp.zeros((window - 1, P_SIZE), jnp.float32), cumulative[:TOKENS + 1 - window]], axis=0)
        recent = jnp.where((widths == window) & (since_start >= window), current - lagged, recent)
    window_mean = recent / jnp.minimum(since_start + 1.0, widths)
    offset = (0.5 * (window_mean + doc_mean) - values).astype(jnp.bfloat16)
    mixed_rows = jnp.einsum('tgc,gcd->tgd', offset.reshape(TOKENS, GROUPS, GROUP_CH).astype(jnp.float32), w_group.astype(jnp.float32)).reshape(TOKENS, P_SIZE)
    mixed_rows = (mixed_rows * pool_scale.astype(jnp.float32)).astype(jnp.bfloat16)
    branch = jnp.dot(mixed_rows, w_branch, preferred_element_type=jnp.float32)
    normed = layer_norm(alpha_mix * resid.astype(jnp.float32) + branch, norm_gain).astype(jnp.bfloat16)
    flat_ids = route_ids.reshape(DEVICES, ROWS * TOPK)
    onehot = (flat_ids[:, :, None] == jnp.arange(EXPERTS, dtype=jnp.int32)[None, None, :]).astype(jnp.int32)
    slot_rank = lax.optimization_barrier(jnp.sum(jnp.cumsum(onehot, axis=1) * onehot, axis=2)) - 1
    block_index = jnp.arange(DEVICES, dtype=jnp.int32)[:, None]
    slot_index = (flat_ids * (DEVICES * CAP) + block_index * CAP + slot_rank).reshape(-1)
    assign_total = TOKENS * TOPK
    source = jnp.full((EXPERTS * DEVICES * CAP,), assign_total, jnp.int32)
    source = source.at[slot_index].set(jnp.arange(assign_total, dtype=jnp.int32)).reshape(EXPERTS, DEVICES * CAP)
    padded = jnp.concatenate([normed, jnp.zeros((1, D), jnp.bfloat16)], axis=0)
    weight_pad = jnp.concatenate([route_wts.reshape(-1), jnp.zeros((1,), jnp.float32)])

    def per_expert(accum, inputs):
        assign_ids, gate_weight, up_weight, down_weight = inputs
        token_ids = assign_ids // TOPK
        hidden = swiglu_hidden(padded[token_ids], gate_weight, up_weight)
        expert_out = jnp.dot(hidden, down_weight, preferred_element_type=jnp.float32).astype(jnp.bfloat16)
        scaled = weight_pad[assign_ids][:, None] * expert_out.astype(jnp.float32)
        return (accum.at[token_ids].add(scaled), None)
    routed, _ = lax.scan(per_expert, jnp.zeros((TOKENS + 1, D), jnp.float32), (source, w_exp_gate, w_exp_up, w_exp_down))
    routed = routed[:TOKENS]
    shared = jnp.dot(swiglu_hidden(normed, w_sh_gate, w_sh_up), w_sh_down, preferred_element_type=jnp.float32)
    return layer_norm(alpha_mix * normed.astype(jnp.float32) + routed + shared, final_gain).astype(jnp.bfloat16)
```

```python
import functools

import jax
import jax.numpy as jnp
from jax import lax
from jax.experimental import pallas as pl
from jax.experimental.pallas import tpu as pltpu
from jax.sharding import PartitionSpec as P

pool_windows = (2, 4, 8, 16, 16, 32, 64, 128)
alpha_mix = 8.0**0.25
norm_eps = 1e-05
halo = max(pool_windows)
MESH = pl.DeviceIdType.MESH
wb_chunks = 4


def layer_norm(values, gain):
    center = values - jnp.mean(values, axis=-1, keepdims=True)
    spread = jnp.mean(center * center, axis=-1, keepdims=True)
    return center * lax.rsqrt(spread + norm_eps) * gain.astype(jnp.float32)


def dot(a, b):
    return jnp.dot(a, b, preferred_element_type=jnp.float32)


def silu_mul(gate, up):
    return (gate / (1.0 + jnp.exp(-gate)) * up).astype(jnp.bfloat16)


def pool_kernel(
    n_sp, n_tp,
    pool_ref, docc_ref, docr_ref, wg_ref, scale_ref, wb_ref, resid_ref, gain_ref,
    out_ref,
    ext, stats, mixed, token_rows, wb_all,
    stat_send, stat_recv, halo_send, halo_recv, mix_send, mix_recv,
    wb_send, wb_recv, fw_send, wb_local,
):
    s, p = lax.axis_index("sp"), lax.axis_index("tp")
    toks, width = pool_ref.shape
    group_width = wg_ref.shape[1]
    rows = resid_ref.shape[0]
    depth = wb_ref.shape[0]
    piece = depth // wb_chunks
    partner = p + 1 - 2 * lax.rem(p, 2)

    barrier = pltpu.get_barrier_semaphore()
    for k in range(1, n_sp):
        pl.semaphore_signal(barrier, inc=1, device_id=(lax.rem(s + k, n_sp), p), device_id_type=MESH)
    for k in range(1, n_tp):
        pl.semaphore_signal(barrier, inc=1, device_id=(s, lax.rem(p + k, n_tp)), device_id_type=MESH)
    pl.semaphore_wait(barrier, n_sp + n_tp - 2)

    def wb_copy(c, src, slot, target, send, recv):
        window = pl.ds(c * piece, piece)
        return pltpu.make_async_remote_copy(
            src_ref=src.at[window], dst_ref=wb_all.at[slot, window],
            send_sem=send, recv_sem=recv, device_id=(s, target), device_id_type=MESH,
        )

    own_wb = pltpu.make_async_copy(wb_ref, wb_all.at[p], wb_local)
    own_wb.start()

    values = pool_ref[...]
    docc, docr = docc_ref[...], docr_ref[...]
    last = jnp.max(docr, axis=1, keepdims=True)
    first = jnp.min(docr, axis=1, keepdims=True).astype(jnp.float32)
    tail = (docr == last).astype(jnp.float32)
    tail_count = jnp.sum(tail, axis=1, keepdims=True)
    sums = dot(jnp.broadcast_to(tail, (8, toks)).astype(jnp.bfloat16), values)
    lane = lax.broadcasted_iota(jnp.int32, (8, 128), 1)
    stats[s, :, 0:width] = sums
    stats[s, :, width : width + 128] = jnp.where(lane == 0, last.astype(jnp.float32), tail_count)

    halo_copy = pltpu.make_async_remote_copy(
        src_ref=pool_ref.at[pl.ds(toks - halo, halo)], dst_ref=ext.at[pl.ds(0, halo)],
        send_sem=halo_send, recv_sem=halo_recv,
        device_id=(lax.rem(s + 1, n_sp), p), device_id_type=MESH,
    )
    halo_copy.start()
    ext[halo:, :] = values

    tpos = lax.broadcasted_iota(jnp.int32, (toks, toks), 0)
    spos = lax.broadcasted_iota(jnp.int32, (toks, toks), 1)
    same = ((docc == docr) & (spos <= tpos)).astype(jnp.float32)
    here = jnp.sum(same, axis=1, keepdims=True)
    running = dot(same.astype(jnp.bfloat16), values)

    stat_copies = []
    for k in range(1, n_sp):
        stat_copies.append(
            pltpu.make_async_remote_copy(
                src_ref=stats.at[s], dst_ref=stats.at[s],
                send_sem=stat_send.at[k], recv_sem=stat_recv.at[k],
                device_id=(lax.rem(s + k, n_sp), p), device_id_type=MESH,
            )
        )
        stat_copies[-1].start()

    cross = []
    for c in range(wb_chunks):
        for j in range(1, n_tp // 2):
            cross.append(
                wb_copy(c, wb_ref, p, lax.rem(p + 2 * j, n_tp), wb_send.at[j, c], wb_recv.at[2 * j, c])
            )
            cross[-1].start()
    beside = [wb_copy(c, wb_ref, p, partner, wb_send.at[0, c], wb_recv.at[1, c]) for c in range(wb_chunks)]
    for copy in beside:
        copy.start()

    for copy in stat_copies:
        copy.wait_recv()
    prev_count = jnp.zeros((1, 1), jnp.float32)
    prev_sums = jnp.zeros((1, width), jnp.float32)
    for k in range(n_sp):
        block = stats[k]
        joined = (block[0:1, width : width + 1] == first) & (k < s)
        prev_count = prev_count + jnp.where(joined, block[0:1, width + 1 : width + 2], 0.0)
        prev_sums = prev_sums + jnp.where(joined, block[0:1, 0:width], 0.0)
    carried = docc.astype(jnp.float32) == first
    length = here + jnp.where(carried, prev_count, 0.0)
    running = running + jnp.where(carried, prev_sums, 0.0)
    doc_mean = running / length

    halo_copy.wait_recv()
    tpos = lax.broadcasted_iota(jnp.int32, (toks, toks + halo), 0) + halo
    spos = lax.broadcasted_iota(jnp.int32, (toks, toks + halo), 1)
    back = tpos - spos
    groups = width // group_width
    for i in range(groups):
        g = p * groups + i
        window = jnp.int32(0)
        for at, size in enumerate(pool_windows):
            window = jnp.where(g == at, size, window)
        span = jnp.minimum(length, window.astype(jnp.float32))
        band = ((back >= 0) & (back < span.astype(jnp.int32))).astype(jnp.float32).astype(jnp.bfloat16)
        cols = slice(i * group_width, (i + 1) * group_width)
        recent = dot(band, ext[:, cols])
        offset = 0.5 * (recent / span + doc_mean[:, cols]) - values[:, cols].astype(jnp.float32)
        turned = dot(offset.astype(jnp.bfloat16), wg_ref[g])
        scale = scale_ref[0:1, pl.ds(pl.multiple_of(g * group_width, group_width), group_width)]
        mixed[:, cols] = (turned * scale.astype(jnp.float32)).astype(jnp.bfloat16)

    mix_copies = []
    for k in range(1, n_tp):
        q = lax.rem(p + k, n_tp)
        mix_copies.append(
            pltpu.make_async_remote_copy(
                src_ref=mixed.at[pl.ds(pl.multiple_of(q * rows, rows), rows)], dst_ref=token_rows.at[p],
                send_sem=mix_send.at[k], recv_sem=mix_recv.at[k],
                device_id=(s, q), device_id_type=MESH,
            )
        )
        mix_copies[-1].start()
    token_rows[p] = mixed[pl.ds(pl.multiple_of(p * rows, rows), rows), :]

    onward = []
    for c in range(wb_chunks):
        for j in range(1, n_tp // 2):
            slot = lax.rem(p - 2 * j + n_tp, n_tp)
            cross[c * (n_tp // 2 - 1) + j - 1].wait_recv()
            onward.append(
                wb_copy(c, wb_all.at[slot], slot, partner, fw_send.at[j, c], wb_recv.at[2 * j + 1, c])
            )
            onward[-1].start()
    for copy in mix_copies:
        copy.wait_recv()
    own_wb.wait()
    for copy in beside + onward:
        copy.wait_recv()
    branch = alpha_mix * resid_ref[...].astype(jnp.float32)
    for k in range(n_tp):
        branch = branch + dot(token_rows[k], wb_all[k])
    out_ref[...] = layer_norm(branch, gain_ref[...]).astype(jnp.bfloat16)
    halo_copy.wait_send()
    for copy in stat_copies + mix_copies + cross + beside + onward:
        copy.wait_send()


def expert_kernel(
    n_sp, n_tp, cap, parts,
    normed_ref, ids_ref, wts_ref, eg_hbm, eu_hbm, ed_hbm, sg_hbm, su_hbm, sd_hbm, gain_ref,
    out_ref,
    eg, eu, ed, sg, su, sd, outgoing, arrived, answers, returned, acc, pick, share,
    load_sem, go_send, go_recv, back_send, back_recv,
):
    n = n_sp * n_tp
    s, p = lax.axis_index("sp"), lax.axis_index("tp")
    me = s * n_tp + p
    toks = normed_ref.shape[0]
    per = n // parts
    span = per * cap

    def place(k):
        d = lax.rem(k, n)
        return (d // n_tp, lax.rem(d, n_tp))

    barrier = pltpu.get_barrier_semaphore()

    @pl.loop(1, n)
    def _(o):
        pl.semaphore_signal(barrier, inc=1, device_id=place(me + o), device_id_type=MESH)

    loads = [
        pltpu.make_async_copy(a, b, load_sem.at[i])
        for i, (a, b) in enumerate(
            [(sg_hbm, sg), (su_hbm, su), (sd_hbm, sd), (eg_hbm.at[0], eg), (eu_hbm.at[0], eu), (ed_hbm.at[0], ed)]
        )
    ]
    for load in loads:
        load.start()

    ahead = lax.broadcasted_iota(jnp.int32, (n, toks), 0)
    chosen = jnp.zeros((n, toks), jnp.float32)
    weight = jnp.zeros((n, toks), jnp.float32)
    for k in range(ids_ref.shape[0]):
        rel = ids_ref[k : k + 1, :] - me
        rel = jnp.where(rel < 0, rel + n, rel)
        hit = ahead == rel
        chosen = chosen + jnp.where(hit, 1.0, 0.0)
        weight = weight + jnp.where(hit, wts_ref[k : k + 1, :], 0.0)
    earlier = lax.broadcasted_iota(jnp.int32, (toks, toks), 0) < lax.broadcasted_iota(jnp.int32, (toks, toks), 1)
    rank = dot(chosen.astype(jnp.bfloat16), earlier.astype(jnp.float32).astype(jnp.bfloat16))
    key = jnp.where(chosen > 0.0, rank, -1.0)
    slot = lax.broadcasted_iota(jnp.int32, (n, cap, toks), 1).astype(jnp.float32)
    taken = slot == key[:, None, :]
    pick[...] = jnp.where(taken, 1.0, 0.0).reshape(n * cap, toks).astype(jnp.bfloat16)
    full = jnp.where(taken, weight[:, None, :], 0.0).reshape(n * cap, toks)
    high = full.astype(jnp.bfloat16)
    share[:, 0:toks] = high
    share[:, toks:] = (full - high.astype(jnp.float32)).astype(jnp.bfloat16)

    def chunk(o):
        return pl.ds(pl.multiple_of(o * cap, cap), cap)

    def part(g):
        return pl.ds(pl.multiple_of(g * span, span), span)

    def go(o):
        return pltpu.make_async_remote_copy(
            src_ref=outgoing.at[chunk(o)], dst_ref=arrived.at[chunk(o)],
            send_sem=go_send.at[o], recv_sem=go_recv.at[o],
            device_id=place(me + o), device_id_type=MESH,
        )

    def back(o):
        return pltpu.make_async_remote_copy(
            src_ref=answers.at[chunk(o)], dst_ref=returned.at[chunk(o)],
            send_sem=back_send.at[o], recv_sem=back_recv.at[o],
            device_id=place(me + n - o), device_id_type=MESH,
        )

    def each(g, act):
        @pl.loop(jnp.maximum(g * per, 1), (g + 1) * per)
        def _(o):
            act(o)

    @pl.loop(0, parts)
    def _(g):
        outgoing[part(g), :] = dot(pick[part(g), :], normed_ref[...]).astype(jnp.bfloat16)

    arrived[0:cap, :] = outgoing[0:cap, :]
    pl.semaphore_wait(barrier, n - 1)

    @pl.loop(1, n)
    def _(o):
        go(o).start()

    normed = normed_ref[...]
    for load in loads[:3]:
        load.wait()
    hidden = silu_mul(dot(normed, sg[...]), dot(normed, su[...]))
    acc[...] = alpha_mix * normed.astype(jnp.float32) + dot(hidden, sd[...])
    for load in loads[3:]:
        load.wait()

    @pl.loop(0, parts)
    def _(g):
        each(g, lambda o: go(o).wait_recv())
        tokens = arrived[part(g), :]
        inner = silu_mul(dot(tokens, eg[...]), dot(tokens, eu[...]))
        answers[part(g), :] = dot(inner, ed[...]).astype(jnp.bfloat16)
        each(g, lambda o: back(o).start())

    returned[0:cap, :] = answers[0:cap, :]

    @pl.loop(0, parts)
    def _(g):
        each(g, lambda o: back(o).wait_recv())
        both = lax.dot_general(
            share[part(g), :], returned[part(g), :], (((0,), (0,)), ((), ())),
            preferred_element_type=jnp.float32,
        )
        acc[...] += both[0:toks] + both[toks:]

    out_ref[...] = layer_norm(acc[...], gain_ref[...]).astype(jnp.bfloat16)

    @pl.loop(1, n)
    def _(o):
        go(o).wait_send()
        back(o).wait_send()


def local(
    n_sp, n_tp,
    resid, pool_in, doc_ids, w_group, pool_scale, w_branch, norm_gain, route_ids, route_wts,
    w_exp_gate, w_exp_up, w_exp_down, w_sh_gate, w_sh_up, w_sh_down, final_gain,
):
    toks, width = pool_in.shape
    rows, model = resid.shape
    depth = w_branch.shape[0]
    n = n_sp * n_tp
    cap = max(16, 2 * rows * route_ids.shape[1] // n)
    parts = 4
    ff = w_sh_gate.shape[1]
    vmem, hbm = pl.BlockSpec(memory_space=pltpu.VMEM), pl.BlockSpec(memory_space=pl.ANY)
    dma = pltpu.SemaphoreType.DMA
    bf16, f32 = jnp.bfloat16, jnp.float32
    normed = pl.pallas_call(
        functools.partial(pool_kernel, n_sp, n_tp),
        out_shape=jax.ShapeDtypeStruct((rows, model), bf16),
        in_specs=[vmem] * 5 + [hbm] + [vmem] * 2,
        out_specs=vmem,
        scratch_shapes=[
            pltpu.VMEM((halo + toks, width), bf16),
            pltpu.VMEM((n_sp, 8, width + 128), f32),
            pltpu.VMEM((toks, width), bf16),
            pltpu.VMEM((n_tp, rows, width), bf16),
            pltpu.VMEM((n_tp, depth, model), bf16),
            dma((n_sp,)), dma((n_sp,)), dma, dma, dma((n_tp,)), dma((n_tp,)),
            dma((n_tp, wb_chunks)), dma((n_tp, wb_chunks)), dma((n_tp, wb_chunks)), dma,
        ],
        compiler_params=pltpu.CompilerParams(
            collective_id=0, has_side_effects=True, vmem_limit_bytes=48 << 20
        ),
        name="pool_mixer",
    )(
        pool_in, doc_ids[:, None], doc_ids[None, :], w_group, pool_scale[None, :], w_branch,
        resid, norm_gain[None, :],
    )
    return pl.pallas_call(
        functools.partial(expert_kernel, n_sp, n_tp, cap, parts),
        out_shape=jax.ShapeDtypeStruct((rows, model), bf16),
        in_specs=[vmem] * 3 + [hbm] * 6 + [vmem],
        out_specs=vmem,
        scratch_shapes=[
            pltpu.VMEM((model, ff), bf16), pltpu.VMEM((model, ff), bf16), pltpu.VMEM((ff, model), bf16),
            pltpu.VMEM((model, ff), bf16), pltpu.VMEM((model, ff), bf16), pltpu.VMEM((ff, model), bf16),
            pltpu.VMEM((n * cap, model), bf16), pltpu.VMEM((n * cap, model), bf16),
            pltpu.VMEM((n * cap, model), bf16), pltpu.VMEM((n * cap, model), bf16),
            pltpu.VMEM((rows, model), f32),
            pltpu.VMEM((n * cap, rows), bf16), pltpu.VMEM((n * cap, 2 * rows), bf16),
            dma((6,)), dma((n,)), dma((n,)), dma((n,)), dma((n,)),
        ],
        compiler_params=pltpu.CompilerParams(
            collective_id=1, has_side_effects=True, vmem_limit_bytes=62 << 20
        ),
        name="routed_experts",
    )(
        normed, route_ids.T, route_wts.T, w_exp_gate, w_exp_up, w_exp_down,
        w_sh_gate, w_sh_up, w_sh_down, final_gain[None, :],
    )


def solution(mesh):
    both = P(("sp", "tp"), None)
    stack = P(("sp", "tp"), None, None)
    placed = (
        both, P("sp", "tp"), P("sp"), P(), P(), P("tp", None), P(), both, both,
        stack, stack, stack, P(), P(), P(), P(),
    )
    return jax.shard_map(
        functools.partial(local, mesh.shape["sp"], mesh.shape["tp"]),
        mesh=mesh, in_specs=placed, out_specs=both, check_vma=False,
    )
```

```python
import functools

import jax
import jax.numpy as jnp
from jax import lax
from jax.experimental import pallas as pl
from jax.experimental.pallas import tpu as pltpu
from jax.sharding import PartitionSpec as P

pool_windows = (2, 4, 8, 16, 16, 32, 64, 128)
alpha_mix = 8.0**0.25
norm_eps = 1e-05
halo = max(pool_windows)
MESH = pl.DeviceIdType.MESH
wb_chunks = 4


def layer_norm(values, gain):
    center = values - jnp.mean(values, axis=-1, keepdims=True)
    spread = jnp.mean(center * center, axis=-1, keepdims=True)
    return center * lax.rsqrt(spread + norm_eps) * gain.astype(jnp.float32)


def dot(a, b):
    return jnp.dot(a, b, preferred_element_type=jnp.float32)


def silu_mul(gate, up):
    return (gate / (1.0 + jnp.exp(-gate)) * up).astype(jnp.bfloat16)


def pool_kernel(
    n_sp, n_tp,
    pool_ref, docc_ref, docr_ref, wg_ref, scale_ref, wb_ref, resid_ref, gain_ref, meta_ref,
    out_ref, metas_ref,
    ext, stats, mixed, token_rows, wb_all,
    stat_send, stat_recv, halo_send, halo_recv, mix_send, mix_recv,
    wb_send, wb_recv, fw_send, wb_local,
):
    s, p = lax.axis_index("sp"), lax.axis_index("tp")
    toks, width = pool_ref.shape
    group_width = wg_ref.shape[1]
    rows = resid_ref.shape[0]
    depth = wb_ref.shape[0]
    piece = depth // wb_chunks
    partner = p + 1 - 2 * lax.rem(p, 2)

    barrier = pltpu.get_barrier_semaphore()
    for k in range(1, n_sp):
        pl.semaphore_signal(barrier, inc=1, device_id=(lax.rem(s + k, n_sp), p), device_id_type=MESH)
    for k in range(1, n_tp):
        pl.semaphore_signal(barrier, inc=1, device_id=(s, lax.rem(p + k, n_tp)), device_id_type=MESH)
    pl.semaphore_wait(barrier, n_sp + n_tp - 2)

    def wb_copy(c, src, slot, target, send, recv):
        window = pl.ds(c * piece, piece)
        return pltpu.make_async_remote_copy(
            src_ref=src.at[window], dst_ref=wb_all.at[slot, window],
            send_sem=send, recv_sem=recv, device_id=(s, target), device_id_type=MESH,
        )

    own_wb = pltpu.make_async_copy(wb_ref, wb_all.at[p], wb_local)
    own_wb.start()

    values = pool_ref[...]
    docc, docr = docc_ref[...], docr_ref[...]
    last = jnp.max(docr, axis=1, keepdims=True)
    first = jnp.min(docr, axis=1, keepdims=True).astype(jnp.float32)
    tail = (docr == last).astype(jnp.float32)
    tail_count = jnp.sum(tail, axis=1, keepdims=True)
    sums = dot(jnp.broadcast_to(tail, (8, toks)).astype(jnp.bfloat16), values)
    lane = lax.broadcasted_iota(jnp.int32, (8, 128), 1)
    stats[s, :, 0:width] = sums
    stats[s, :, width + 128 :] = meta_ref[...]
    stats[s, :, width : width + 128] = jnp.where(lane == 0, last.astype(jnp.float32), tail_count)

    halo_copy = pltpu.make_async_remote_copy(
        src_ref=pool_ref.at[pl.ds(toks - halo, halo)], dst_ref=ext.at[pl.ds(0, halo)],
        send_sem=halo_send, recv_sem=halo_recv,
        device_id=(lax.rem(s + 1, n_sp), p), device_id_type=MESH,
    )
    halo_copy.start()
    ext[halo:, :] = values

    tpos = lax.broadcasted_iota(jnp.int32, (toks, toks), 0)
    spos = lax.broadcasted_iota(jnp.int32, (toks, toks), 1)
    same = ((docc == docr) & (spos <= tpos)).astype(jnp.float32)
    here = jnp.sum(same, axis=1, keepdims=True)
    running = dot(same.astype(jnp.bfloat16), values)

    stat_copies = []
    for k in range(1, n_sp):
        stat_copies.append(
            pltpu.make_async_remote_copy(
                src_ref=stats.at[s], dst_ref=stats.at[s],
                send_sem=stat_send.at[k], recv_sem=stat_recv.at[k],
                device_id=(lax.rem(s + k, n_sp), p), device_id_type=MESH,
            )
        )
        stat_copies[-1].start()

    cross = []
    for c in range(wb_chunks):
        for j in range(1, n_tp // 2):
            cross.append(
                wb_copy(c, wb_ref, p, lax.rem(p + 2 * j, n_tp), wb_send.at[j, c], wb_recv.at[2 * j, c])
            )
            cross[-1].start()
    beside = [wb_copy(c, wb_ref, p, partner, wb_send.at[0, c], wb_recv.at[1, c]) for c in range(wb_chunks)]
    for copy in beside:
        copy.start()

    for copy in stat_copies:
        copy.wait_recv()
    prev_count = jnp.zeros((1, 1), jnp.float32)
    prev_sums = jnp.zeros((1, width), jnp.float32)
    for k in range(n_sp):
        block = stats[k]
        joined = (block[0:1, width : width + 1] == first) & (k < s)
        prev_count = prev_count + jnp.where(joined, block[0:1, width + 1 : width + 2], 0.0)
        prev_sums = prev_sums + jnp.where(joined, block[0:1, 0:width], 0.0)
    carried = docc.astype(jnp.float32) == first
    length = here + jnp.where(carried, prev_count, 0.0)
    running = running + jnp.where(carried, prev_sums, 0.0)
    doc_mean = running / length

    halo_copy.wait_recv()
    tpos = lax.broadcasted_iota(jnp.int32, (toks, toks + halo), 0) + halo
    spos = lax.broadcasted_iota(jnp.int32, (toks, toks + halo), 1)
    back = tpos - spos
    groups = width // group_width
    for i in range(groups):
        g = p * groups + i
        window = jnp.int32(0)
        for at, size in enumerate(pool_windows):
            window = jnp.where(g == at, size, window)
        span = jnp.minimum(length, window.astype(jnp.float32))
        band = ((back >= 0) & (back < span.astype(jnp.int32))).astype(jnp.float32).astype(jnp.bfloat16)
        cols = slice(i * group_width, (i + 1) * group_width)
        recent = dot(band, ext[:, cols])
        offset = 0.5 * (recent / span + doc_mean[:, cols]) - values[:, cols].astype(jnp.float32)
        turned = dot(offset.astype(jnp.bfloat16), wg_ref[g])
        scale = scale_ref[0:1, pl.ds(pl.multiple_of(g * group_width, group_width), group_width)]
        mixed[:, cols] = (turned * scale.astype(jnp.float32)).astype(jnp.bfloat16)

    mix_copies = []
    for k in range(1, n_tp):
        q = lax.rem(p + k, n_tp)
        mix_copies.append(
            pltpu.make_async_remote_copy(
                src_ref=mixed.at[pl.ds(pl.multiple_of(q * rows, rows), rows)], dst_ref=token_rows.at[p],
                send_sem=mix_send.at[k], recv_sem=mix_recv.at[k],
                device_id=(s, q), device_id_type=MESH,
            )
        )
        mix_copies[-1].start()
    token_rows[p] = mixed[pl.ds(pl.multiple_of(p * rows, rows), rows), :]

    onward = []
    for c in range(wb_chunks):
        for j in range(1, n_tp // 2):
            slot = lax.rem(p - 2 * j + n_tp, n_tp)
            cross[c * (n_tp // 2 - 1) + j - 1].wait_recv()
            onward.append(
                wb_copy(c, wb_all.at[slot], slot, partner, fw_send.at[j, c], wb_recv.at[2 * j + 1, c])
            )
            onward[-1].start()
    for copy in mix_copies:
        copy.wait_recv()
    own_wb.wait()
    for copy in beside + onward:
        copy.wait_recv()
    branch = alpha_mix * resid_ref[...].astype(jnp.float32)
    for k in range(n_tp):
        branch = branch + dot(token_rows[k], wb_all[k])
    out_ref[...] = layer_norm(branch, gain_ref[...]).astype(jnp.bfloat16)
    metas_ref[...] = stats[:, :, width + 128 :]
    halo_copy.wait_send()
    for copy in stat_copies + mix_copies + cross + beside + onward:
        copy.wait_send()


def expert_kernel(
    n_sp, n_tp, n_x, cap,
    normed_ref, metas_ref, eg_hbm, eu_hbm, ed_hbm, sg_hbm, su_hbm, sd_hbm, gain_ref,
    out_ref,
    eg, eu, ed, sg, su, sd, blocks, outgoing, arrived, returned, column, across, chain, acc, pick, share,
    load_sem, up_send, down_send, x_send, block_recv, go_send, go_recv, back_send, back_recv,
    across_send, across_recv, chain_send, chain_recv,
):
    n_z = n_sp // n_x
    s, p = lax.axis_index("sp"), lax.axis_index("tp")
    z, x = s // n_x, lax.rem(s, n_x)
    toks = normed_ref.shape[0]
    top = metas_ref.shape[1] // 2

    barrier = pltpu.get_barrier_semaphore()
    for k in range(1, n_sp):
        pl.semaphore_signal(barrier, inc=1, device_id=(lax.rem(s + k, n_sp), p), device_id_type=MESH)
    for k in range(1, n_tp):
        pl.semaphore_signal(barrier, inc=1, device_id=(s, lax.rem(p + k, n_tp)), device_id_type=MESH)

    loads = [
        pltpu.make_async_copy(a, b, load_sem.at[i])
        for i, (a, b) in enumerate(
            [(sg_hbm, sg), (su_hbm, su), (sd_hbm, sd), (eg_hbm.at[0], eg), (eu_hbm.at[0], eu), (ed_hbm.at[0], ed)]
        )
    ]
    for load in loads:
        load.start()
    blocks[s] = normed_ref[...]

    low = jnp.minimum(z, n_z - 1 - z)
    rising = jnp.where(z * 2 < n_z, 1, -1)
    near = [z]
    for i in range(1, n_z):
        swing = z - (i + 1) // 2 if i % 2 else z + i // 2
        near.append(jnp.where(2 * low >= i, swing, z + rising * (i - low)))

    def copy(src, dst, send, recv, where):
        return pltpu.make_async_remote_copy(
            src_ref=src, dst_ref=dst, send_sem=send, recv_sem=recv, device_id=where, device_id_type=MESH
        )

    def up(zb):
        k = zb * n_x + x
        return copy(blocks.at[k], blocks.at[k], up_send.at[zb], block_recv.at[k], (jnp.minimum(s + n_x, n_sp - 1), p))

    def down(zb):
        k = zb * n_x + x
        return copy(blocks.at[k], blocks.at[k], down_send.at[zb], block_recv.at[k], (jnp.maximum(s - n_x, 0), p))

    def beside(zb, o):
        k = zb * n_x + x
        where = (z * n_x + lax.rem(x + o, n_x), p)
        return copy(blocks.at[k], blocks.at[k], x_send.at[zb, o], block_recv.at[k], where)

    def arrival(k):
        where = (lax.rem(s + 1, n_sp), p)
        return copy(blocks.at[k], blocks.at[k], x_send.at[0, 0], block_recv.at[k], where)

    def rises(zb):
        return (zb <= z) & (z + 1 < n_z)

    def sinks(zb):
        return (zb >= z) & (z > 0)

    def relay(zb):
        @pl.when(rises(zb))
        def _():
            up(zb).start()

        @pl.when(sinks(zb))
        def _():
            down(zb).start()

        for o in range(1, n_x):
            beside(zb, o).start()

    def seat(j):
        return pl.ds(j * cap, cap)

    def go(k, j):
        return copy(
            outgoing.at[k, seat(j)], arrived.at[k, seat(j)], go_send.at[k, j], go_recv.at[k, j],
            (s, lax.rem(p + j, n_tp)),
        )

    def back(k, j):
        return copy(
            arrived.at[k, seat(j)], returned.at[k, seat(j)], back_send.at[k, j], back_recv.at[k, j],
            (s, lax.rem(p + n_tp - j, n_tp)),
        )

    def send_partial(zb, o):
        xb = lax.rem(x + o, n_x)
        k = zb * n_x + xb
        return copy(
            blocks.at[k], across.at[zb, o], across_send.at[zb, o], across_recv.at[zb, o], (z * n_x + xb, p)
        )

    def index(i, o):
        return near[i] * n_x + lax.rem(x + o, n_x)

    def dispatch(i, o):
        k = index(i, o)
        if i or o:
            arrival(k).wait_recv()
            if not o:
                relay(near[i])
        outgoing[k] = dot(pick[k], blocks[k]).astype(jnp.bfloat16)
        for j in range(1, n_tp):
            go(k, j).start()
        arrived[k, seat(0)] = outgoing[k, seat(0)]

    def experts(i, o):
        k = index(i, o)
        for j in range(1, n_tp):
            go(k, j).wait_recv()
        tokens = arrived[k]
        inner = silu_mul(dot(tokens, eg[...]), dot(tokens, eu[...]))
        arrived[k] = dot(inner, ed[...]).astype(jnp.bfloat16)
        for j in range(1, n_tp):
            back(k, j).start()
        returned[k, seat(0)] = arrived[k, seat(0)]

    def combine(i, o):
        k = index(i, o)
        for j in range(1, n_tp):
            back(k, j).wait_recv()
        both = lax.dot_general(
            share[k], returned[k], (((0,), (0,)), ((), ())), preferred_element_type=jnp.float32
        )
        partial = both[0:toks] + both[toks:]
        if o:
            blocks[k] = partial.astype(jnp.bfloat16)
            send_partial(near[i], o).start()
        else:
            column[near[i]] = partial

    pl.semaphore_wait(barrier, n_sp + n_tp - 2)
    relay(z)

    pad = -(-n_tp // 8) * 8
    expert = s * n_tp + lax.rem(p + lax.broadcasted_iota(jnp.int32, (n_sp, pad, toks), 1), n_tp)
    expert = expert.astype(jnp.float32)
    chosen = jnp.zeros((n_sp, pad, toks), jnp.float32)
    weight = jnp.zeros((n_sp, pad, toks), jnp.float32)
    for a in range(top):
        hit = metas_ref[:, a : a + 1, :] == expert
        chosen = chosen + jnp.where(hit, 1.0, 0.0)
        weight = weight + jnp.where(hit, metas_ref[:, top + a : top + a + 1, :], 0.0)
    earlier = lax.broadcasted_iota(jnp.int32, (toks, toks), 0) < lax.broadcasted_iota(jnp.int32, (toks, toks), 1)
    rank = dot(
        chosen.reshape(n_sp * pad, toks).astype(jnp.bfloat16), earlier.astype(jnp.float32).astype(jnp.bfloat16)
    ).reshape(n_sp, pad, toks)
    key = jnp.where(chosen > 0.0, rank, -1.0)
    slot = lax.broadcasted_iota(jnp.int32, (n_sp, cap, toks), 1).astype(jnp.float32)
    for j in range(n_tp):
        taken = slot == key[:, j : j + 1, :]
        pick[:, seat(j), :] = jnp.where(taken, 1.0, 0.0).astype(jnp.bfloat16)
        full = jnp.where(taken, weight[:, j : j + 1, :], 0.0)
        high = full.astype(jnp.bfloat16)
        share[:, seat(j), 0:toks] = high
        share[:, seat(j), toks:] = (full - high.astype(jnp.float32)).astype(jnp.bfloat16)

    order = [(0, 0)]
    for i in range(1, n_z):
        order += [(i, 0)] + [(i - 1, o) for o in range(1, n_x)]
    order += [(n_z - 1, o) for o in range(1, n_x)]
    for at in range(len(order) + 3):
        if at < len(order):
            dispatch(*order[at])
        if at == 0:
            for load in loads[:3]:
                load.wait()
            hidden = silu_mul(dot(normed_ref[...], sg[...]), dot(normed_ref[...], su[...]))
            acc[...] = alpha_mix * normed_ref[...].astype(jnp.float32) + dot(hidden, sd[...])
            for load in loads[3:]:
                load.wait()
        if 0 <= at - 1 < len(order):
            experts(*order[at - 1])
        if 0 <= at - 3 < len(order):
            combine(*order[at - 3])

    for zb in range(n_z):
        @pl.when(rises(zb))
        def _():
            up(zb).wait_send()

        @pl.when(sinks(zb))
        def _():
            down(zb).wait_send()

        for o in range(1, n_x):
            beside(zb, o).wait_send()

    def column_sum(zb):
        total = column[zb]
        for o in range(1, n_x):
            send_partial(zb, o).wait_recv()
            total = total + across[zb, o].astype(jnp.float32)
        column[zb] = total

    def link(side, zb):
        where = s + n_x if side == 0 else s - n_x
        where = jnp.maximum(jnp.minimum(where, n_sp - 1), 0)
        return copy(
            blocks.at[zb * n_x + x], chain.at[side, zb], chain_send.at[zb], chain_recv.at[side, zb], (where, p)
        )

    def take(side, zb, holds):
        @pl.when(holds)
        def _():
            link(side, zb).wait_recv()
            column[zb] += chain[side, zb].astype(jnp.float32)

    for i in range(n_z - 1, 0, -1):
        zb = near[i]
        column_sum(zb)
        take(0, zb, (zb > z) & (z > 0))
        take(1, zb, (zb < z) & (z + 1 < n_z))
        blocks[zb * n_x + x] = column[zb].astype(jnp.bfloat16)

        @pl.when(zb > z)
        def _():
            link(0, zb).start()

        @pl.when(zb < z)
        def _():
            link(1, zb).start()

    column_sum(z)
    take(0, z, z > 0)
    take(1, z, z + 1 < n_z)
    out_ref[...] = layer_norm(acc[...] + column[z], gain_ref[...]).astype(jnp.bfloat16)

    for i in range(1, n_z):
        link(0, near[i]).wait_send()
    for k in range(n_sp):
        for j in range(1, n_tp):
            go(k, j).wait_send()
            back(k, j).wait_send()
    for zb in range(n_z):
        for o in range(1, n_x):
            send_partial(zb, o).wait_send()


def local(
    n_sp, n_tp,
    resid, pool_in, doc_ids, w_group, pool_scale, w_branch, norm_gain, route_ids, route_wts,
    w_exp_gate, w_exp_up, w_exp_down, w_sh_gate, w_sh_up, w_sh_down, final_gain,
):
    toks, width = pool_in.shape
    rows, model = resid.shape
    depth = w_branch.shape[0]
    cap = 2 * rows * route_ids.shape[1] // (n_sp * n_tp)
    n_x = max(k for k in range(1, n_sp + 1) if n_sp % k == 0 and k * k <= n_sp)
    n_z = n_sp // n_x
    ff = w_sh_gate.shape[1]
    meta = jnp.concatenate([route_ids.astype(jnp.float32), route_wts], axis=1).T
    vmem, hbm = pl.BlockSpec(memory_space=pltpu.VMEM), pl.BlockSpec(memory_space=pl.ANY)
    dma = pltpu.SemaphoreType.DMA
    bf16, f32 = jnp.bfloat16, jnp.float32
    normed, metas = pl.pallas_call(
        functools.partial(pool_kernel, n_sp, n_tp),
        out_shape=(
            jax.ShapeDtypeStruct((rows, model), bf16),
            jax.ShapeDtypeStruct((n_sp, meta.shape[0], rows), f32),
        ),
        in_specs=[vmem] * 5 + [hbm] + [vmem] * 3,
        out_specs=(vmem, vmem),
        scratch_shapes=[
            pltpu.VMEM((halo + toks, width), bf16),
            pltpu.VMEM((n_sp, 8, width + 128 + rows), f32),
            pltpu.VMEM((toks, width), bf16),
            pltpu.VMEM((n_tp, rows, width), bf16),
            pltpu.VMEM((n_tp, depth, model), bf16),
            dma((n_sp,)), dma((n_sp,)), dma, dma, dma((n_tp,)), dma((n_tp,)),
            dma((n_tp, wb_chunks)), dma((n_tp, wb_chunks)), dma((n_tp, wb_chunks)), dma,
        ],
        compiler_params=pltpu.CompilerParams(
            collective_id=0, has_side_effects=True, vmem_limit_bytes=48 << 20
        ),
        name="pool_mixer",
    )(
        pool_in, doc_ids[:, None], doc_ids[None, :], w_group, pool_scale[None, :], w_branch,
        resid, norm_gain[None, :], meta,
    )
    seats = pltpu.VMEM((n_sp, n_tp * cap, model), bf16)
    block = (rows, model)
    return pl.pallas_call(
        functools.partial(expert_kernel, n_sp, n_tp, n_x, cap),
        out_shape=jax.ShapeDtypeStruct(block, bf16),
        in_specs=[vmem] * 2 + [hbm] * 6 + [vmem],
        out_specs=vmem,
        scratch_shapes=[
            pltpu.VMEM((model, ff), bf16), pltpu.VMEM((model, ff), bf16), pltpu.VMEM((ff, model), bf16),
            pltpu.VMEM((model, ff), bf16), pltpu.VMEM((model, ff), bf16), pltpu.VMEM((ff, model), bf16),
            pltpu.VMEM((n_sp, *block), bf16),
            seats, seats, seats,
            pltpu.VMEM((n_z, *block), f32),
            pltpu.VMEM((n_z, n_x, *block), bf16),
            pltpu.VMEM((2, n_z, *block), bf16),
            pltpu.VMEM(block, f32),
            pltpu.VMEM((n_sp, n_tp * cap, rows), bf16), pltpu.VMEM((n_sp, n_tp * cap, 2 * rows), bf16),
            dma((6,)), dma((n_z,)), dma((n_z,)), dma((n_z, n_x)), dma((n_sp,)),
            dma((n_sp, n_tp)), dma((n_sp, n_tp)), dma((n_sp, n_tp)), dma((n_sp, n_tp)),
            dma((n_z, n_x)), dma((n_z, n_x)), dma((n_z,)), dma((2, n_z)),
        ],
        compiler_params=pltpu.CompilerParams(
            collective_id=1, has_side_effects=True, vmem_limit_bytes=62 << 20
        ),
        name="routed_experts",
    )(
        normed, metas, w_exp_gate, w_exp_up, w_exp_down,
        w_sh_gate, w_sh_up, w_sh_down, final_gain[None, :],
    )


def solution(mesh):
    both = P(("sp", "tp"), None)
    stack = P(("sp", "tp"), None, None)
    placed = (
        both, P("sp", "tp"), P("sp"), P(), P(), P("tp", None), P(), both, both,
        stack, stack, stack, P(), P(), P(), P(),
    )
    return jax.shard_map(
        functools.partial(local, mesh.shape["sp"], mesh.shape["tp"]),
        mesh=mesh, in_specs=placed, out_specs=both, check_vma=False,
    )
```
